128 devices in a mesh: sp: 32 (over z, y, core), tp: 4 (over x).
Axes of the slice: x: 4, y: 4, z: 4, core: 2. Of those that a mesh axis runs over, the one named last changes fastest.
Arguments:
- tokens: bfloat16 [4, 2048, 1024], P(None, 'sp', 'tp'), may hold values from -6 to 6
- norm_gain: float32 [4, 1024], replicated, may hold values from 0.1 to 1.9
- val_weight: bfloat16 [4, 1024, 512], P(None, 'sp', 'tp'), may hold values from -0.1875 to 0.1875
- gate_weight: bfloat16 [4, 1024, 512], P(None, 'sp', 'tp'), may hold values from -0.1875 to 0.1875
- conv_taps: float32 [4, 31, 512], P(None, None, 'tp'), may hold values from -1 to 1
- conv_bias: float32 [4, 512], P(None, 'tp'), may hold values from -3 to 3
- ln_gain: float32 [4, 512], P(None, 'tp'), may hold values from 0.1 to 1.9
- ln_shift: float32 [4, 512], P(None, 'tp'), may hold values from -3 to 3
- out_weight: bfloat16 [4, 512, 1024], P(None, 'tp', 'sp'), may hold values from -0.25 to 0.25
Outputs:
- stream: bfloat16 [4, 2048, 1024], P(None, 'sp', 'tp')
The draws below stay inside these ranges and needn't reach their ends.
All inputs are finite; a program needn't handle non-finite values.
Results may differ from the reference program's by a relative error of at most 0.02.
Values may be sent and summed in bfloat16 or wider, within the bound.
A program may use at most 64 MiB of HBM per device.

```python
import jax
import jax.numpy as jnp
from jax import lax

D = 1024
CHANNELS = 512
TAPS = 31
LAYERS = 4
SEQS = 4
TOKENS = 2048


def level_of(stream_key, dims, shards, low, top_value):
    level = 1.0
    for axis_at, shards_of in shards:
        heights = jax.random.uniform(jax.random.fold_in(jax.random.fold_in(stream_key, 6), axis_at), (shards_of,), jnp.float32, low / len(shards), top_value / len(shards))
        level = level * jnp.repeat(jnp.exp(heights), dims[axis_at] // shards_of).reshape((-1,) + (1,) * (len(dims) - 1 - axis_at))
    return level


def normal_values(own_key, shape, scale, most, shards=(), dtype=jnp.bfloat16):
    result = scale * jax.random.normal(own_key, shape, jnp.float32)
    if shards:
        result = result * level_of(own_key, shape, shards, -0.22, 0.18)
    return jnp.clip(result, -most, most).astype(dtype)


def setup_inputs(seed: int = 0) -> dict:
    splits = jax.random.split(jax.random.key(seed), 10)
    tokens = normal_values(splits[0], (SEQS, TOKENS, D), 1.0, 6.0, ((1, 32), (2, 4)))
    norm_gain = jnp.clip(1.0 + 0.18 * jax.random.normal(splits[1], (LAYERS, D), jnp.float32), 0.1, 1.9)
    val_weight = normal_values(splits[2], (LAYERS, D, CHANNELS), D ** -0.5, 0.1875, ((1, 32), (2, 4)))
    gate_weight = normal_values(splits[3], (LAYERS, D, CHANNELS), D ** -0.5, 0.1875, ((1, 32), (2, 4)))
    conv_taps = normal_values(splits[4], (LAYERS, TAPS, CHANNELS), TAPS ** -0.5, 1.0, ((2, 4),), jnp.float32)
    conv_bias = normal_values(splits[5], (LAYERS, CHANNELS), 0.5, 3.0, ((1, 4),), jnp.float32)
    ln_gain = jnp.clip(1.0 + 0.18 * jax.random.normal(splits[6], (LAYERS, CHANNELS), jnp.float32), 0.1, 1.9)
    ln_shift = normal_values(splits[7], (LAYERS, CHANNELS), 0.5, 3.0, ((1, 4),), jnp.float32)
    out_weight = normal_values(splits[8], (LAYERS, CHANNELS, D), CHANNELS ** -0.5, 0.25, ((1, 4), (2, 32)))
    return {"tokens": tokens, "norm_gain": norm_gain, "val_weight": val_weight, "gate_weight": gate_weight, "conv_taps": conv_taps, "conv_bias": conv_bias, "ln_gain": ln_gain, "ln_shift": ln_shift, "out_weight": out_weight}


epsilon = 1e-06

def depthwise(padded, tap_weights, length):
    running = padded[:, 0:length] * tap_weights[0]
    for tap_idx in range(1, tap_weights.shape[0]):
        running = running + padded[:, tap_idx:tap_idx + length] * tap_weights[tap_idx]
    return running

def reference(tokens, norm_gain, val_weight, gate_weight, conv_taps, conv_bias, ln_gain, ln_shift, out_weight):
    stream = tokens
    half_width = TAPS // 2
    for layer_idx in range(LAYERS):
        widened = stream.astype(jnp.float32)
        scaled = widened * jax.lax.rsqrt(lax.optimization_barrier(jnp.mean(widened * widened, axis=-1, keepdims=True)) + epsilon)
        normed = (scaled * norm_gain[layer_idx]).astype(jnp.bfloat16)
        tok_rows = normed.reshape(-1, D)
        values = jnp.dot(tok_rows, val_weight[layer_idx], preferred_element_type=jnp.float32)
        gates = jnp.dot(tok_rows, gate_weight[layer_idx], preferred_element_type=jnp.float32)
        gated = (values * jax.nn.sigmoid(gates)).astype(jnp.bfloat16).reshape(SEQS, TOKENS, CHANNELS)
        padded = jnp.pad(gated.astype(jnp.float32), ((0, 0), (half_width, half_width), (0, 0)))
        convolved = depthwise(padded, conv_taps[layer_idx], TOKENS) + conv_bias[layer_idx]
        mean_val = lax.optimization_barrier(jnp.mean(convolved, axis=-1, keepdims=True))
        centered = convolved - mean_val
        spread = lax.optimization_barrier(jnp.mean(centered * centered, axis=-1, keepdims=True))
        normalized = centered * jax.lax.rsqrt(spread + epsilon) * ln_gain[layer_idx] + ln_shift[layer_idx]
        activated = jax.nn.silu(normalized).astype(jnp.bfloat16).reshape(-1, CHANNELS)
        branch = jnp.dot(activated, out_weight[layer_idx], preferred_element_type=jnp.float32)
        stream = (stream.astype(jnp.float32) + branch.reshape(SEQS, TOKENS, D)).astype(jnp.bfloat16)
    return stream
```

```python
import jax
import jax.numpy as jnp
from jax import lax
from jax.experimental import pallas as pl
from jax.experimental.pallas import tpu as pltpu
from jax.sharding import PartitionSpec as P

MESH = pl.DeviceIdType.MESH
LAYERS = 4
TAPS = 31
HALF = 15
EPS = 1e-6
LOCAL = 64
ROWS = 192
STEP = 16
ORDERS = (("x", "y", "z"), ("y", "z", "x"), ("z", "x", "y"))
F32 = jnp.float32
BF16 = jnp.bfloat16


def kernel(
    tokens, norm_gain, val_w, gate_w, out_w, taps, bias, ln_gain, ln_shift, out,
    w, x_buf, g_buf, c_buf, nb, tap_all, vec_all,
    load_sem, send_sem, first_sem, rest_sem, sib_send, sib_recv, tok_sem, par_sem, end_sem,
):
    sp = lax.axis_index("sp")
    x = lax.axis_index("tp")
    z = sp // 8
    y = (sp // 2) % 4
    c = sp % 2
    at = {"x": x, "y": y, "z": z}
    sibling = (sp + 1 - 2 * c, x)

    def near(axis, step):
        if axis == "x":
            return (sp, (x + step) % 4)
        if axis == "y":
            return (z * 8 + ((y + step) % 4) * 2 + c, x)
        return (((z + step) % 4) * 8 + y * 2 + c, x)

    before = ((sp + 31) % 32, x)
    after = ((sp + 1) % 32, x)
    outer = ((sp + 32 + (2 * c - 1)) % 32, x)

    loads = []
    for k, array in enumerate((val_w, gate_w, out_w)):
        d1, d2, d3 = ORDERS[k]
        loads.append(
            pltpu.make_async_copy(
                array, w.at[:, k, c, at[d3], at[d2], at[d1]], load_sem.at[k]
            )
        )
    loads.append(pltpu.make_async_copy(taps, tap_all.at[x], load_sem.at[3]))
    for j, array in enumerate((bias, ln_gain, ln_shift)):
        loads.append(pltpu.make_async_copy(array, vec_all.at[x, j], load_sem.at[4 + j]))
    own_cols = pl.ds(pl.multiple_of(x * 256, 256), 256)
    loads.append(
        pltpu.make_async_copy(
            tokens.at[x], x_buf.at[pl.ds(LOCAL, LOCAL), own_cols], load_sem.at[7]
        )
    )
    for load in loads:
        load.start()

    barrier = pltpu.get_barrier_semaphore()
    peers = [near(a, s) for a in "xyz" for s in (1, 3)] + [near("x", 2), sibling, outer]
    for peer in peers:
        pl.semaphore_signal(barrier, inc=1, device_id=peer, device_id_type=MESH)
    pl.semaphore_wait(barrier, len(peers))

    def send(ref, dst, peer, s_sem, r_sem):
        pltpu.make_async_remote_copy(
            src_ref=ref, dst_ref=dst, send_sem=s_sem, recv_sem=r_sem,
            device_id=peer, device_id_type=MESH,
        ).start()

    def wait_bytes(ref, sem):
        pltpu.make_async_copy(ref, ref, sem).wait()

    def block(k, phase, layer, index, half):
        d1, d2, d3 = ORDERS[k]
        if phase == 2:
            part = slice(None) if half is None else pl.ds(2 * half, 2)
            return w.at[layer, k, c, index, part]
        part = slice(None) if half is None else pl.ds(2 * half, 2)
        if phase == 0:
            return w.at[part, k, c, at[d3], at[d2], index]
        return w.at[part, k, c, at[d3], index]

    def sems(k, phase, layer):
        return (k, phase if phase < 2 else 2 + layer)

    def own_half(k, phase, layer, which):
        axis = ORDERS[k][phase]
        q, s = sems(k, phase, layer)
        for way, half in ((0, which), (1, 1 - which)):
            ref = block(k, phase, layer, at[axis], half)
            r_sem = first_sem.at[q, s, way] if which == 0 else rest_sem.at[q, s]
            send(ref, ref, near(axis, 1 if way == 0 else 3), send_sem.at[q, s], r_sem)

    def relay(k, phase, layer):
        axis = ORDERS[k][phase]
        q, s = sems(k, phase, layer)
        for way in (0, 1):
            source = (at[axis] + (3 if way == 0 else 1)) % 4
            ref = block(k, phase, layer, source, way)
            wait_bytes(ref, first_sem.at[q, s, way])
            send(
                ref, ref, near(axis, 1 if way == 0 else 3),
                send_sem.at[q, s], rest_sem.at[q, s],
            )

    def span(k, phase, layer, count):
        if phase == 2:
            return w.at[layer, k, 0, pl.ds(0, count)]
        if phase == 0:
            return w.at[:, k, 0, 0, 0, pl.ds(0, count)]
        return w.at[:, k, 0, 0, pl.ds(0, count)]

    def rest(k, phase, layer):
        q, s = sems(k, phase, layer)
        wait_bytes(span(k, phase, layer, 2), rest_sem.at[q, s])

    for k in range(3):
        loads[k].wait()
        own_half(k, 0, 0, 0)
        own_half(k, 0, 0, 1)

    for step in (1, 3, 2):
        other = (x + step) % 4
        send(
            tokens.at[other], x_buf.at[pl.ds(LOCAL, LOCAL), own_cols], (sp, other),
            tok_sem.at[0], tok_sem.at[1],
        )
    for load in loads[3:]:
        load.wait()
    for step in (1, 3, 2):
        other = (x + step) % 4
        send(vec_all.at[x], vec_all.at[x], (sp, other), par_sem.at[0], par_sem.at[1])
        send(tap_all.at[x], tap_all.at[x], (sp, other), par_sem.at[2], par_sem.at[3])

    for k in range(3):
        relay(k, 0, 0)
    for k in range(3):
        rest(k, 0, 0)
        own_half(k, 1, 0, 0)
        own_half(k, 1, 0, 1)

    own_rows = pl.ds(LOCAL, LOCAL)
    wait_bytes(x_buf.at[own_rows, pl.ds(0, 768)], tok_sem.at[1])
    send(x_buf.at[own_rows], x_buf.at[pl.ds(2 * LOCAL, LOCAL)], before, tok_sem.at[2], tok_sem.at[3])
    send(x_buf.at[own_rows], x_buf.at[pl.ds(0, LOCAL)], after, tok_sem.at[4], tok_sem.at[5])

    for k in range(3):
        relay(k, 1, 0)
    for k in range(3):
        rest(k, 1, 0)
        own_half(k, 2, 0, 0)
    for k in range(3):
        own_half(k, 2, 0, 1)
    for k in range(3):
        own_half(k, 2, 1, 0)

    def to_sibling(k, layer, index):
        ref = w.at[layer, k, c, index]
        send(ref, ref, sibling, sib_send.at[layer, k], sib_recv.at[layer, k])

    def advance(layer):
        for k in range(3):
            relay(k, 2, layer)
        for k in range(3):
            if layer + 1 < LAYERS:
                own_half(k, 2, layer + 1, 1)
        for k in range(3):
            if layer + 2 < LAYERS:
                own_half(k, 2, layer + 2, 0)
        for k in range(3):
            to_sibling(k, layer, at[ORDERS[k][2]])

    def finish(layer):
        for k in range(3):
            rest(k, 2, layer)
            for step in (1, 2, 3):
                to_sibling(k, layer, (at[ORDERS[k][2]] + step) % 4)

    def arrived(layer):
        for k in range(3):
            wait_bytes(w.at[layer, k, 0], sib_recv.at[layer, k])

    def weight(layer, k, bz, cols):
        def piece(by, bc, bx):
            index = {"x": bx, "y": by, "z": bz}
            d1, d2, d3 = ORDERS[k]
            return w[layer, k, bc, index[d3], index[d2], index[d1]]

        return jnp.concatenate(
            [
                jnp.concatenate([piece(by, bc, bx) for by in range(4) for bc in range(2)], axis=0)
                for bx in cols
            ],
            axis=1,
        )

    def compute(layer):
        r0 = STEP * layer
        n = ROWS - 2 * r0
        m = n - 2 * STEP
        xs = x_buf[pl.ds(r0, n), :].astype(F32)
        scale = lax.rsqrt(jnp.mean(xs * xs, axis=-1, keepdims=True) + EPS)
        nb[pl.ds(0, n), :] = (xs * scale * norm_gain[pl.ds(layer, 1), :]).astype(BF16)
        token = sp * LOCAL - LOCAL + r0 + lax.broadcasted_iota(jnp.int32, (n, 256), 0)
        inside = jnp.logical_and(token >= 0, token < 32 * LOCAL)
        for half in range(2):
            cols = (2 * half, 2 * half + 1)
            val = jnp.zeros((n, 256), F32)
            gate = jnp.zeros((n, 256), F32)
            for bz in range(4):
                left = nb[pl.ds(0, n), pl.ds(bz * 256, 256)]
                val = val + jnp.dot(left, weight(layer, 0, bz, cols), preferred_element_type=F32)
                gate = gate + jnp.dot(left, weight(layer, 1, bz, cols), preferred_element_type=F32)
            gated = (val * jax.nn.sigmoid(gate)).astype(BF16).astype(F32)
            g_buf[pl.ds(0, n), pl.ds(half * 256, 256)] = jnp.where(inside, gated, 0.0)
        for bx in range(4):
            lanes = pl.ds(bx * 128, 128)
            g = g_buf[pl.ds(0, n), lanes]
            total = jnp.zeros((m, 128), F32) + vec_all[bx, 0, pl.ds(layer, 1), :]
            for shift in range(8):
                moved = g if shift == 0 else pltpu.roll(g, n - shift, 0)
                for k in range(TAPS):
                    if (k + 1) % 8 == shift:
                        base = (k + 1) // 8 * 8
                        total = total + moved[base : base + m] * tap_all[bx, k, pl.ds(layer, 1), :]
            c_buf[pl.ds(0, m), lanes] = total
        conv = c_buf[pl.ds(0, m), :]
        mean = jnp.mean(conv, axis=-1, keepdims=True)
        centred = conv - mean
        spread = jnp.mean(centred * centred, axis=-1, keepdims=True)
        gain = jnp.concatenate([vec_all[bx, 1, pl.ds(layer, 1), :] for bx in range(4)], axis=1)
        shift = jnp.concatenate([vec_all[bx, 2, pl.ds(layer, 1), :] for bx in range(4)], axis=1)
        normalized = centred * lax.rsqrt(spread + EPS) * gain + shift
        act = jax.nn.silu(normalized).astype(BF16)
        rows = pl.ds(r0 + STEP, m)
        for bz in range(4):
            branch = lax.dot_general(
                act, weight(layer, 2, bz, range(4)), (((1,), (1,)), ((), ())),
                preferred_element_type=F32,
            )
            lanes = pl.ds(bz * 256, 256)
            x_buf[rows, lanes] = (x_buf[rows, lanes].astype(F32) + branch).astype(BF16)

    advance(0)
    finish(0)
    advance(1)
    wait_bytes(vec_all.at[pl.ds(0, 3)], par_sem.at[1])
    wait_bytes(tap_all.at[pl.ds(0, 3)], par_sem.at[3])
    wait_bytes(x_buf.at[own_rows], tok_sem.at[2])
    wait_bytes(x_buf.at[own_rows], tok_sem.at[3])
    wait_bytes(x_buf.at[own_rows], tok_sem.at[4])
    wait_bytes(x_buf.at[own_rows], tok_sem.at[5])
    arrived(0)
    compute(0)
    advance(2)
    finish(1)
    arrived(1)
    compute(1)
    advance(3)
    finish(2)
    arrived(2)
    compute(2)
    finish(3)
    arrived(3)
    compute(3)

    for step in (1, 3, 2):
        other = (x + step) % 4
        cols = pl.ds(pl.multiple_of(other * 256, 256), 256)
        send(x_buf.at[own_rows, cols], out.at[x], (sp, other), end_sem.at[0], end_sem.at[1])
    out[x] = x_buf[own_rows, own_cols]

    for k in range(3):
        for phase in range(2):
            wait_bytes(span(k, phase, 0, 3), send_sem.at[k, phase])
        for layer in range(LAYERS):
            wait_bytes(span(k, 2, layer, 3), send_sem.at[k, 2 + layer])
            wait_bytes(w.at[layer, k, 0], sib_send.at[layer, k])
    wait_bytes(out.at[pl.ds(0, 3)], tok_sem.at[0])
    wait_bytes(vec_all.at[pl.ds(0, 3)], par_sem.at[0])
    wait_bytes(tap_all.at[pl.ds(0, 3)], par_sem.at[2])
    wait_bytes(out.at[pl.ds(0, 3)], end_sem.at[0])
    wait_bytes(out.at[pl.ds(0, 3)], end_sem.at[1])


def shards(tokens, norm_gain, val_w, gate_w, taps, bias, ln_gain, ln_shift, out_w):
    hbm = pl.BlockSpec(memory_space=pl.ANY)
    vmem = pl.BlockSpec(memory_space=pltpu.VMEM)
    dma = pltpu.SemaphoreType.DMA
    return pl.pallas_call(
        kernel,
        out_shape=jax.ShapeDtypeStruct(tokens.shape, BF16),
        in_specs=[hbm, vmem] + [hbm] * 7,
        out_specs=vmem,
        scratch_shapes=[
            pltpu.VMEM((LAYERS, 3, 2, 4, 4, 4, 32, 128), BF16),
            pltpu.VMEM((ROWS, 1024), BF16),
            pltpu.VMEM((ROWS, 512), F32),
            pltpu.VMEM((ROWS, 512), F32),
            pltpu.VMEM((ROWS, 1024), BF16),
            pltpu.VMEM((4, TAPS, LAYERS, 128), F32),
            pltpu.VMEM((4, 3, LAYERS, 128), F32),
            dma((8,)),
            dma((3, 6)),
            dma((3, 6, 2)),
            dma((3, 6)),
            dma((LAYERS, 3)),
            dma((LAYERS, 3)),
            dma((6,)),
            dma((4,)),
            dma((2,)),
        ],
        compiler_params=pltpu.CompilerParams(collective_id=0, has_side_effects=True),
    )(
        tokens, norm_gain, val_w, gate_w, jnp.swapaxes(out_w, 1, 2),
        jnp.swapaxes(taps, 0, 1), bias, ln_gain, ln_shift,
    )


def solution(mesh):
    return jax.shard_map(
        shards,
        mesh=mesh,
        in_specs=(
            P(None, "sp", "tp"),
            P(),
            P(None, "sp", "tp"),
            P(None, "sp", "tp"),
            P(None, None, "tp"),
            P(None, "tp"),
            P(None, "tp"),
            P(None, "tp"),
            P(None, "tp", "sp"),
        ),
        out_specs=P(None, "sp", "tp"),
        check_vma=False,
    )
```

```python
import jax
import jax.numpy as jnp
from jax import lax
from jax.experimental import pallas as pl
from jax.experimental.pallas import tpu as pltpu
from jax.sharding import PartitionSpec as P

MESH = pl.DeviceIdType.MESH
LAYERS = 4
TAPS = 31
EPS = 1e-6
LOCAL = 64
ROWS = 192
STEP = 16
ORDERS = (("x", "y", "z"), ("y", "z", "x"), ("z", "x", "y"))
SEMS = 200
F32 = jnp.float32
BF16 = jnp.bfloat16


def kernel(
    tokens, norm_gain, val_w, gate_w, out_w, taps, bias, ln_gain, ln_shift, out,
    w, x_buf, g_buf, c_buf, nb, gains, tap_in, tap_bf, tap_all, vec_all, y_buf, sem,
):
    sp = lax.axis_index("sp")
    x = lax.axis_index("tp")
    z = sp // 8
    y = (sp // 2) % 4
    c = sp % 2
    at = {"x": x, "y": y, "z": z}
    sibling = (sp + 1 - 2 * c, x)
    used = []

    def new_sem():
        used.append(0)
        return sem.at[len(used) - 1]

    def near(axis, step):
        if axis == "x":
            return (sp, (x + step) % 4)
        if axis == "y":
            return (z * 8 + ((y + step) % 4) * 2 + c, x)
        return (((z + step) % 4) * 8 + y * 2 + c, x)

    before = ((sp + 31) % 32, x)
    after = ((sp + 1) % 32, x)
    outer = ((sp + 31 + 2 * c) % 32, x)

    def send(ref, dst, peer, s_sem, r_sem):
        pltpu.make_async_remote_copy(
            src_ref=ref, dst_ref=dst, send_sem=s_sem, recv_sem=r_sem,
            device_id=peer, device_id_type=MESH,
        ).start()

    def wait_bytes(ref, a_sem):
        pltpu.make_async_copy(ref, ref, a_sem).wait()

    sent = []

    own_cols = pl.ds(pl.multiple_of(x * 256, 256), 256)
    own_rows = pl.ds(LOCAL, LOCAL)

    def load(src, dst):
        copy = pltpu.make_async_copy(src, dst, new_sem())
        copy.start()
        return copy

    loads = []
    for k, array in enumerate((val_w, gate_w, out_w)):
        d1, d2, d3 = ORDERS[k]
        loads.append(load(array, w.at[:, k, c, at[d3], at[d2], at[d1]]))
    tap_load = load(taps, tap_in)
    small_loads = [
        load(array, vec_all.at[x, j]) for j, array in enumerate((bias, ln_gain, ln_shift))
    ]
    token_load = load(tokens.at[x], x_buf.at[own_rows, own_cols])
    gain_load = load(norm_gain, gains)

    barrier = pltpu.get_barrier_semaphore()
    peers = [near(a, s) for a in "xyz" for s in (1, 3, 2)] + [sibling, outer]
    for peer in peers:
        pl.semaphore_signal(barrier, inc=1, device_id=peer, device_id_type=MESH)

    tap_load.wait()
    for layer in range(LAYERS):
        tap_bf[x, layer] = jnp.concatenate(
            [tap_in[:, layer, :], jnp.zeros((1, 128), F32)], axis=0
        ).astype(BF16)
    for k in range(3):
        loads[k].wait()
    pl.semaphore_wait(barrier, len(peers))

    def block(k, phase, layer, index):
        d1, d2, d3 = ORDERS[k]
        if phase == 0:
            return w.at[layer, k, c, at[d3], at[d2], index]
        if phase == 1:
            return w.at[layer, k, c, at[d3], index]
        return w.at[layer, k, c, index]

    def many(k, phase, layer, count):
        if phase == 0:
            return w.at[layer, k, 0, 0, 0, pl.ds(0, count)]
        if phase == 1:
            return w.at[layer, k, 0, 0, pl.ds(0, count)]
        return w.at[layer, k, 0, pl.ds(0, count)]

    def direct(phase, layer):
        waits = []
        for k in range(3):
            s_sem, r_sem = new_sem(), new_sem()
            axis = ORDERS[k][phase]
            ref = block(k, phase, layer, at[axis])
            for step in (2, 1, 3):
                send(ref, ref, near(axis, step), s_sem, r_sem)
            sent.append((many(k, phase, layer, 3), s_sem))
            waits.append((many(k, phase, layer, 3), r_sem))

        def wait():
            for ref, r_sem in waits:
                wait_bytes(ref, r_sem)

        return wait

    first_sems = [[[new_sem(), new_sem()] for k in range(3)] for l in range(LAYERS)]
    second_sems = [[new_sem() for k in range(3)] for l in range(LAYERS)]
    relay_sems = [[new_sem() for k in range(3)] for l in range(LAYERS)]
    ring_send = [[new_sem() for k in range(3)] for l in range(LAYERS)]
    sib_send = [[new_sem() for k in range(3)] for l in range(LAYERS)]
    sib_recv = [[new_sem() for k in range(3)] for l in range(LAYERS)]
    for l in range(LAYERS):
        for k in range(3):
            sent.append((many(k, 2, l, 3), ring_send[l][k]))
            sent.append((many(k, 2, l, 4), sib_send[l][k]))

    def half_block(k, layer, index, half):
        return w.at[layer, k, c, index, pl.ds(2 * half, 2)]

    def to_sibling(k, layer, ref):
        send(ref, ref, sibling, sib_send[layer][k], sib_recv[layer][k])

    def own(layer, which):
        for k in range(3):
            axis = ORDERS[k][2]
            for way in (0, 1):
                half = which if way == 0 else 1 - which
                ref = half_block(k, layer, at[axis], half)
                r_sem = first_sems[layer][k][way] if which == 0 else second_sems[layer][k]
                send(ref, ref, near(axis, 1 if way == 0 else 3), ring_send[layer][k], r_sem)

    def relay(layer):
        for k in range(3):
            axis = ORDERS[k][2]
            for way in (0, 1):
                step = 1 if way == 0 else 3
                ref = half_block(k, layer, (at[axis] + 4 - step) % 4, way)
                wait_bytes(ref, first_sems[layer][k][way])
                send(ref, ref, near(axis, step), ring_send[layer][k], relay_sems[layer][k])

    def share_own(layer):
        for k in range(3):
            to_sibling(k, layer, block(k, 2, layer, at[ORDERS[k][2]]))

    def share_first(layer):
        for k in range(3):
            axis = ORDERS[k][2]
            for way in (0, 1):
                to_sibling(k, layer, half_block(k, layer, (at[axis] + (3, 1)[way]) % 4, way))

    def share_second(layer):
        for k in range(3):
            axis = ORDERS[k][2]
            wait_bytes(many(k, 2, layer, 1), second_sems[layer][k])
            for way in (0, 1):
                to_sibling(k, layer, half_block(k, layer, (at[axis] + (3, 1)[way]) % 4, 1 - way))

    def share_relay(layer):
        for k in range(3):
            axis = ORDERS[k][2]
            wait_bytes(many(k, 2, layer, 1), relay_sems[layer][k])
            to_sibling(k, layer, block(k, 2, layer, (at[axis] + 2) % 4))

    def arrived(layer):
        for k in range(3):
            wait_bytes(many(k, 2, layer, 4), sib_recv[layer][k])

    def weight(layer, k, bz, cols):
        def piece(by, bc, bx):
            index = {"x": bx, "y": by, "z": bz}
            d1, d2, d3 = ORDERS[k]
            return w[layer, k, bc, index[d3], index[d2], index[d1]]

        return jnp.concatenate(
            [
                jnp.concatenate([piece(by, bc, bx) for by in range(4) for bc in range(2)], axis=0)
                for bx in cols
            ],
            axis=1,
        )

    def branch(layer, act, bz):
        return lax.dot_general(
            act, weight(layer, 2, bz, range(4)), (((1,), (1,)), ((), ())),
            preferred_element_type=F32,
        )

    def activated(layer):
        r0 = STEP * layer
        n = ROWS - 2 * r0
        m = n - 2 * STEP
        xs = x_buf[pl.ds(r0, n), :].astype(F32)
        scale = lax.rsqrt(jnp.mean(xs * xs, axis=-1, keepdims=True) + EPS)
        nb[pl.ds(0, n), :] = (xs * scale * gains[pl.ds(layer, 1), :]).astype(BF16)
        token = sp * LOCAL - LOCAL + r0 + lax.broadcasted_iota(jnp.int32, (n, 256), 0)
        inside = jnp.logical_and(token >= 0, token < 32 * LOCAL)
        for half in range(2):
            cols = (2 * half, 2 * half + 1)
            val = jnp.zeros((n, 256), F32)
            gate = jnp.zeros((n, 256), F32)
            for bz in range(4):
                left = nb[pl.ds(0, n), pl.ds(bz * 256, 256)]
                val = val + jnp.dot(left, weight(layer, 0, bz, cols), preferred_element_type=F32)
                gate = gate + jnp.dot(left, weight(layer, 1, bz, cols), preferred_element_type=F32)
            gated = (val * jax.nn.sigmoid(gate)).astype(BF16).astype(F32)
            g_buf[pl.ds(0, n), pl.ds(half * 256, 256)] = jnp.where(inside, gated, 0.0)
        for bx in range(4):
            lanes = pl.ds(bx * 128, 128)
            g = g_buf[pl.ds(0, n), lanes]
            total = jnp.zeros((m, 128), F32) + vec_all[bx, 0, pl.ds(layer, 1), :]
            for shift in range(8):
                moved = g if shift == 0 else pltpu.roll(g, n - shift, 0)
                for k in range(TAPS):
                    if (k + 1) % 8 == shift:
                        base = (k + 1) // 8 * 8
                        total = total + moved[base : base + m] * tap_all[bx, layer, pl.ds(k, 1), :]
            c_buf[pl.ds(0, m), lanes] = total
        conv = c_buf[pl.ds(0, m), :]
        mean = jnp.mean(conv, axis=-1, keepdims=True)
        centred = conv - mean
        spread = jnp.mean(centred * centred, axis=-1, keepdims=True)
        gain = jnp.concatenate([vec_all[bx, 1, pl.ds(layer, 1), :] for bx in range(4)], axis=1)
        shift = jnp.concatenate([vec_all[bx, 2, pl.ds(layer, 1), :] for bx in range(4)], axis=1)
        normalized = centred * lax.rsqrt(spread + EPS) * gain + shift
        return jax.nn.silu(normalized).astype(BF16)

    def compute(layer):
        act = activated(layer)
        rows = pl.ds(STEP * (layer + 1), ROWS - 2 * STEP * (layer + 1))
        for bz in range(4):
            lanes = pl.ds(bz * 256, 256)
            x_buf[rows, lanes] = (x_buf[rows, lanes].astype(F32) + branch(layer, act, bz)).astype(BF16)

    ph0_first = direct(0, pl.ds(0, 1))
    ph0_later = direct(0, pl.ds(1, 3))

    tok_send, tok_recv = new_sem(), new_sem()
    for step in (2, 1, 3):
        other = (x + step) % 4
        send(tokens.at[other], x_buf.at[own_rows, own_cols], (sp, other), tok_send, tok_recv)
    sent.append((x_buf.at[own_rows, pl.ds(0, 768)], tok_send))
    own_taps = pl.ds(2 * c, 2)
    par_sems = [new_sem() for _ in range(6)]
    for copy in small_loads:
        copy.wait()
    for step in (2, 1, 3):
        other = (x + step) % 4
        send(tap_bf.at[x, own_taps], tap_bf.at[x, own_taps], (sp, other), par_sems[0], par_sems[1])
        send(vec_all.at[x], vec_all.at[x], (sp, other), par_sems[2], par_sems[3])
    sent.append((tap_bf.at[pl.ds(0, 3), pl.ds(0, 2)], par_sems[0]))
    sent.append((vec_all.at[pl.ds(0, 3)], par_sems[2]))

    ph0_first()
    ph1 = [direct(1, pl.ds(0, 1))]
    ph0_later()
    ph1.append(direct(1, pl.ds(1, 1)))
    ph1.append(direct(1, pl.ds(2, 1)))
    ph1.append(direct(1, pl.ds(3, 1)))

    token_load.wait()
    wait_bytes(x_buf.at[own_rows, pl.ds(0, 768)], tok_recv)
    halo = [new_sem() for _ in range(4)]
    send(x_buf.at[own_rows], x_buf.at[pl.ds(2 * LOCAL, LOCAL)], before, halo[0], halo[1])
    send(x_buf.at[own_rows], x_buf.at[pl.ds(0, LOCAL)], after, halo[2], halo[3])
    wait_bytes(tap_bf.at[pl.ds(0, 3), pl.ds(0, 2)], par_sems[1])
    for step in (1, 2, 3):
        other = (x + step) % 4
        ref = tap_bf.at[other, own_taps]
        send(ref, ref, sibling, par_sems[4], par_sems[5])
    sent.append((tap_bf.at[pl.ds(0, 3), pl.ds(0, 2)], par_sems[4]))

    ph1[0]()
    own(0, 0)
    own(0, 1)
    share_own(0)
    ph1[1]()
    own(1, 0)
    relay(0)
    share_first(0)
    own(1, 1)
    share_own(1)
    ph1[2]()
    own(2, 0)
    share_second(0)
    share_relay(0)
    relay(1)
    share_first(1)
    own(2, 1)
    share_own(2)
    ph1[3]()
    own(3, 0)

    wait_bytes(vec_all.at[pl.ds(0, 3)], par_sems[3])
    wait_bytes(tap_bf.at[pl.ds(0, 3), pl.ds(0, 2)], par_sems[5])
    tap_all[...] = tap_bf[...].astype(F32)
    gain_load.wait()
    for a_sem in halo:
        wait_bytes(x_buf.at[own_rows], a_sem)

    arrived(0)
    compute(0)
    share_second(1)
    share_relay(1)
    relay(2)
    share_first(2)
    own(3, 1)
    share_own(3)
    arrived(1)
    compute(1)
    share_second(2)
    share_relay(2)
    relay(3)
    share_first(3)
    arrived(2)
    compute(2)
    share_second(3)
    share_relay(3)
    arrived(3)

    act = activated(3)
    end_send, end_recv = new_sem(), new_sem()
    for i, step in enumerate((2, 1, 3, 0)):
        other = (x + step) % 4
        cols = pl.ds(pl.multiple_of(other * 256, 256), 256)
        result = (x_buf[own_rows, cols].astype(F32) + branch(3, act, other)).astype(BF16)
        if step:
            y_buf[i] = result
            send(y_buf.at[i], out.at[x], (sp, other), end_send, end_recv)
        else:
            out[x] = result
    sent.append((y_buf.at[pl.ds(0, 3)], end_send))
    wait_bytes(y_buf.at[pl.ds(0, 3)], end_recv)
    for ref, a_sem in sent:
        wait_bytes(ref, a_sem)


def shards(tokens, norm_gain, val_w, gate_w, taps, bias, ln_gain, ln_shift, out_w):
    hbm = pl.BlockSpec(memory_space=pl.ANY)
    vmem = pl.BlockSpec(memory_space=pltpu.VMEM)
    return pl.pallas_call(
        kernel,
        out_shape=pltpu.VMEM(tokens.shape, BF16),
        in_specs=[hbm] * 9,
        out_specs=vmem,
        scratch_shapes=[
            pltpu.VMEM((LAYERS, 3, 2, 4, 4, 4, 32, 128), BF16),
            pltpu.VMEM((ROWS, 1024), BF16),
            pltpu.VMEM((ROWS, 512), F32),
            pltpu.VMEM((ROWS, 512), F32),
            pltpu.VMEM((ROWS, 1024), BF16),
            pltpu.VMEM((LAYERS, 1024), F32),
            pltpu.VMEM((TAPS, LAYERS, 128), F32),
            pltpu.VMEM((4, LAYERS, 32, 128), BF16),
            pltpu.VMEM((4, LAYERS, 32, 128), F32),
            pltpu.VMEM((4, 3, LAYERS, 128), F32),
            pltpu.VMEM((3, LOCAL, 256), BF16),
            pltpu.SemaphoreType.DMA((SEMS,)),
        ],
        compiler_params=pltpu.CompilerParams(collective_id=0, has_side_effects=True),
    )(
        tokens, norm_gain, val_w, gate_w, jnp.swapaxes(out_w, 1, 2),
        jnp.swapaxes(taps, 0, 1), bias, ln_gain, ln_shift,
    )


def solution(mesh):
    return jax.shard_map(
        shards,
        mesh=mesh,
        in_specs=(
            P(None, "sp", "tp"),
            P(),
            P(None, "sp", "tp"),
            P(None, "sp", "tp"),
            P(None, None, "tp"),
            P(None, "tp"),
            P(None, "tp"),
            P(None, "tp"),
            P(None, "tp", "sp"),
        ),
        out_specs=P(None, "sp", "tp"),
        check_vma=False,
    )
```

```python
import jax
import jax.numpy as jnp
from jax import lax
from jax.experimental import pallas as pl
from jax.experimental.pallas import tpu as pltpu
from jax.sharding import PartitionSpec as P

MESH = pl.DeviceIdType.MESH
LAYERS = 4
TAPS = 31
EPS = 1e-6
LOCAL = 64
ROWS = 192
STEP = 16
CYCLE = ("xyz", "yzx", "zxy")
ORDERS = (CYCLE, CYCLE, CYCLE, CYCLE)
SEMS = 280
F32 = jnp.float32
BF16 = jnp.bfloat16


def kernel(
    tokens, norm_gain, val_w, gate_w, out_w, taps, bias, ln_gain, ln_shift, out,
    w, x_buf, g_buf, c_buf, nb, gains, tap_in, tap_bf, tap_all, vec_all, y_buf, sem,
):
    sp = lax.axis_index("sp")
    x = lax.axis_index("tp")
    z = sp // 8
    y = (sp // 2) % 4
    c = sp % 2
    at = {"x": x, "y": y, "z": z}
    sibling = (sp + 1 - 2 * c, x)
    used = []

    def new_sem():
        used.append(0)
        return sem.at[len(used) - 1]

    def near(axis, step):
        if axis == "x":
            return (sp, (x + step) % 4)
        if axis == "y":
            return (z * 8 + ((y + step) % 4) * 2 + c, x)
        return (((z + step) % 4) * 8 + y * 2 + c, x)

    before = ((sp + 31) % 32, x)
    after = ((sp + 1) % 32, x)
    outer = ((sp + 31 + 2 * c) % 32, x)

    def send(ref, dst, peer, s_sem, r_sem):
        pltpu.make_async_remote_copy(
            src_ref=ref, dst_ref=dst, send_sem=s_sem, recv_sem=r_sem,
            device_id=peer, device_id_type=MESH,
        ).start()

    def wait_bytes(ref, a_sem):
        pltpu.make_async_copy(ref, ref, a_sem).wait()

    sent = []

    own_cols = pl.ds(pl.multiple_of(x * 256, 256), 256)
    own_rows = pl.ds(LOCAL, LOCAL)

    def load(src, dst):
        copy = pltpu.make_async_copy(src, dst, new_sem())
        copy.start()
        return copy

    loads = []
    for layer in range(LAYERS):
        for k, array in enumerate((val_w, gate_w, out_w)):
            d1, d2, d3 = ORDERS[layer][k]
            loads.append(load(array.at[layer], w.at[layer, k, c, at[d3], at[d2], at[d1]]))
    tap_load = load(taps, tap_in)
    small_loads = [
        load(array, vec_all.at[x, j]) for j, array in enumerate((bias, ln_gain, ln_shift))
    ]
    token_load = load(tokens.at[x], x_buf.at[own_rows, own_cols])
    gain_load = load(norm_gain, gains)

    barrier = pltpu.get_barrier_semaphore()
    peers = [near(a, s) for a in "xyz" for s in (1, 3, 2)] + [sibling, outer]
    for peer in peers:
        pl.semaphore_signal(barrier, inc=1, device_id=peer, device_id_type=MESH)

    tap_load.wait()
    for layer in range(LAYERS):
        tap_bf[x, layer] = jnp.concatenate(
            [tap_in[:, layer, :], jnp.zeros((1, 128), F32)], axis=0
        ).astype(BF16)
    for copy in loads:
        copy.wait()
    pl.semaphore_wait(barrier, len(peers))

    def block(k, phase, layer, index):
        d1, d2, d3 = ORDERS[layer][k]
        if phase == 0:
            return w.at[layer, k, c, at[d3], at[d2], index]
        if phase == 1:
            return w.at[layer, k, c, at[d3], index]
        return w.at[layer, k, c, index]

    def many(k, phase, layer, count):
        if phase == 0:
            return w.at[layer, k, 0, 0, 0, pl.ds(0, count)]
        if phase == 1:
            return w.at[layer, k, 0, 0, pl.ds(0, count)]
        return w.at[layer, k, 0, pl.ds(0, count)]

    def direct(phase, layer):
        waits = []
        for k in range(3):
            s_sem, r_sem = new_sem(), new_sem()
            axis = ORDERS[layer][k][phase]
            ref = block(k, phase, layer, at[axis])
            for step in (2, 1, 3):
                send(ref, ref, near(axis, step), s_sem, r_sem)
            sent.append((many(k, phase, layer, 3), s_sem))
            waits.append((many(k, phase, layer, 3), r_sem))

        def wait():
            for ref, r_sem in waits:
                wait_bytes(ref, r_sem)

        return wait

    line_sems = [[[new_sem(), new_sem()] for k in range(3)] for l in range(LAYERS)]
    line_rest = [[new_sem() for k in range(3)] for l in range(LAYERS)]
    line_send = [[new_sem() for k in range(3)] for l in range(LAYERS)]

    def line_half(k, layer, index, half):
        d1, d2, d3 = ORDERS[layer][k]
        return w.at[layer, k, c, at[d3], index, pl.ds(2 * half, 2)]

    def line_own(layer):
        for which in (0, 1):
            for k in range(3):
                axis = ORDERS[layer][k][1]
                for way in (0, 1):
                    half = which if way == 0 else 1 - which
                    ref = line_half(k, layer, at[axis], half)
                    r_sem = line_sems[layer][k][way] if which == 0 else line_rest[layer][k]
                    send(ref, ref, near(axis, 1 if way == 0 else 3), line_send[layer][k], r_sem)
        for k in range(3):
            sent.append((many(k, 1, layer, 3), line_send[layer][k]))

    def line_relay(layer):
        for k in range(3):
            axis = ORDERS[layer][k][1]
            for way in (0, 1):
                step = 1 if way == 0 else 3
                ref = line_half(k, layer, (at[axis] + 4 - step) % 4, way)
                wait_bytes(ref, line_sems[layer][k][way])
                send(ref, ref, near(axis, step), line_send[layer][k], line_rest[layer][k])

    def line_wait(layer):
        for k in range(3):
            wait_bytes(many(k, 1, layer, 2), line_rest[layer][k])

    first_sems = [[[new_sem(), new_sem()] for k in range(3)] for l in range(LAYERS)]
    second_sems = [[new_sem() for k in range(3)] for l in range(LAYERS)]
    relay_sems = [[new_sem() for k in range(3)] for l in range(LAYERS)]
    ring_send = [[new_sem() for k in range(3)] for l in range(LAYERS)]
    sib_send = [[new_sem() for k in range(3)] for l in range(LAYERS)]
    sib_recv = [[new_sem() for k in range(3)] for l in range(LAYERS)]
    for l in range(LAYERS):
        for k in range(3):
            sent.append((many(k, 2, l, 3), ring_send[l][k]))
            sent.append((many(k, 2, l, 4), sib_send[l][k]))

    def half_block(k, layer, index, half):
        return w.at[layer, k, c, index, pl.ds(2 * half, 2)]

    def to_sibling(k, layer, ref):
        send(ref, ref, sibling, sib_send[layer][k], sib_recv[layer][k])

    def own(layer, which):
        for k in range(3):
            axis = ORDERS[layer][k][2]
            for way in (0, 1):
                half = which if way == 0 else 1 - which
                ref = half_block(k, layer, at[axis], half)
                r_sem = first_sems[layer][k][way] if which == 0 else second_sems[layer][k]
                send(ref, ref, near(axis, 1 if way == 0 else 3), ring_send[layer][k], r_sem)

    def relay(layer):
        for k in range(3):
            axis = ORDERS[layer][k][2]
            for way in (0, 1):
                step = 1 if way == 0 else 3
                ref = half_block(k, layer, (at[axis] + 4 - step) % 4, way)
                wait_bytes(ref, first_sems[layer][k][way])
                send(ref, ref, near(axis, step), ring_send[layer][k], relay_sems[layer][k])

    def share_own(layer):
        for k in range(3):
            to_sibling(k, layer, block(k, 2, layer, at[ORDERS[layer][k][2]]))

    def share_first(layer):
        for k in range(3):
            axis = ORDERS[layer][k][2]
            for way in (0, 1):
                to_sibling(k, layer, half_block(k, layer, (at[axis] + (3, 1)[way]) % 4, way))

    def share_second(layer):
        for k in range(3):
            axis = ORDERS[layer][k][2]
            wait_bytes(many(k, 2, layer, 1), second_sems[layer][k])
            for way in (0, 1):
                to_sibling(k, layer, half_block(k, layer, (at[axis] + (3, 1)[way]) % 4, 1 - way))

    def share_relay(layer):
        for k in range(3):
            axis = ORDERS[layer][k][2]
            wait_bytes(many(k, 2, layer, 1), relay_sems[layer][k])
            to_sibling(k, layer, block(k, 2, layer, (at[axis] + 2) % 4))

    def arrived(layer):
        for k in range(3):
            wait_bytes(many(k, 2, layer, 4), sib_recv[layer][k])

    def weight(layer, k, bz, cols):
        def piece(by, bc, bx):
            index = {"x": bx, "y": by, "z": bz}
            d1, d2, d3 = ORDERS[layer][k]
            return w[layer, k, bc, index[d3], index[d2], index[d1]]

        return jnp.concatenate(
            [
                jnp.concatenate([piece(by, bc, bx) for by in range(4) for bc in range(2)], axis=0)
                for bx in cols
            ],
            axis=1,
        )

    def branch(layer, act, bz):
        return lax.dot_general(
            act, weight(layer, 2, bz, range(4)), (((1,), (1,)), ((), ())),
            preferred_element_type=F32,
        )

    def activated(layer, middle):
        r0 = STEP * layer
        n = ROWS - 2 * r0
        m = n - 2 * STEP
        xs = x_buf[pl.ds(r0, n), :].astype(F32)
        scale = lax.rsqrt(jnp.mean(xs * xs, axis=-1, keepdims=True) + EPS)
        nb[pl.ds(0, n), :] = (xs * scale * gains[pl.ds(layer, 1), :]).astype(BF16)
        token = sp * LOCAL - LOCAL + r0 + lax.broadcasted_iota(jnp.int32, (n, 256), 0)
        inside = jnp.logical_and(token >= 0, token < 32 * LOCAL)
        for half in range(2):
            cols = (2 * half, 2 * half + 1)
            val = jnp.zeros((n, 256), F32)
            gate = jnp.zeros((n, 256), F32)
            for bz in range(4):
                left = nb[pl.ds(0, n), pl.ds(bz * 256, 256)]
                val = val + jnp.dot(left, weight(layer, 0, bz, cols), preferred_element_type=F32)
                gate = gate + jnp.dot(left, weight(layer, 1, bz, cols), preferred_element_type=F32)
            gated = (val * jax.nn.sigmoid(gate)).astype(BF16).astype(F32)
            g_buf[pl.ds(0, n), pl.ds(half * 256, 256)] = jnp.where(inside, gated, 0.0)
        for bx in range(4):
            lanes = pl.ds(bx * 128, 128)
            g = g_buf[pl.ds(0, n), lanes]
            total = jnp.zeros((m, 128), F32) + vec_all[bx, 0, pl.ds(layer, 1), :]
            for shift in range(8):
                moved = g if shift == 0 else pltpu.roll(g, n - shift, 0)
                for k in range(TAPS):
                    if (k + 1) % 8 == shift:
                        base = (k + 1) // 8 * 8
                        total = total + moved[base : base + m] * tap_all[bx, layer, pl.ds(k, 1), :]
            c_buf[pl.ds(0, m), lanes] = total
        middle()
        conv = c_buf[pl.ds(0, m), :]
        mean = jnp.mean(conv, axis=-1, keepdims=True)
        centred = conv - mean
        spread = jnp.mean(centred * centred, axis=-1, keepdims=True)
        gain = jnp.concatenate([vec_all[bx, 1, pl.ds(layer, 1), :] for bx in range(4)], axis=1)
        shift = jnp.concatenate([vec_all[bx, 2, pl.ds(layer, 1), :] for bx in range(4)], axis=1)
        normalized = centred * lax.rsqrt(spread + EPS) * gain + shift
        return jax.nn.silu(normalized).astype(BF16)

    def compute(layer, middle):
        act = activated(layer, middle)
        rows = pl.ds(STEP * (layer + 1), ROWS - 2 * STEP * (layer + 1))
        for bz in range(4):
            lanes = pl.ds(bz * 256, 256)
            x_buf[rows, lanes] = (x_buf[rows, lanes].astype(F32) + branch(layer, act, bz)).astype(BF16)

    ph0 = [direct(0, layer) for layer in range(LAYERS)]

    tok_send, tok_recv = new_sem(), new_sem()
    for step in (2, 1, 3):
        other = (x + step) % 4
        send(tokens.at[other], x_buf.at[own_rows, own_cols], (sp, other), tok_send, tok_recv)
    sent.append((x_buf.at[own_rows, pl.ds(0, 768)], tok_send))
    own_taps = pl.ds(2 * c, 2)
    par_sems = [new_sem() for _ in range(6)]
    for copy in small_loads:
        copy.wait()
    for step in (2, 1, 3):
        other = (x + step) % 4
        send(tap_bf.at[x, own_taps], tap_bf.at[x, own_taps], (sp, other), par_sems[0], par_sems[1])
        send(vec_all.at[x], vec_all.at[x], (sp, other), par_sems[2], par_sems[3])
    sent.append((tap_bf.at[pl.ds(0, 3), pl.ds(0, 2)], par_sems[0]))
    sent.append((vec_all.at[pl.ds(0, 3)], par_sems[2]))

    ph1 = []
    for layer in range(LAYERS):
        ph0[layer]()
        if layer in (2, 3):
            line_own(layer)
            ph1.append(lambda layer=layer: line_wait(layer))
        else:
            ph1.append(direct(1, layer))

    token_load.wait()
    wait_bytes(x_buf.at[own_rows, pl.ds(0, 768)], tok_recv)
    halo = [new_sem() for _ in range(4)]
    send(x_buf.at[own_rows], x_buf.at[pl.ds(2 * LOCAL, LOCAL)], before, halo[0], halo[1])
    send(x_buf.at[own_rows], x_buf.at[pl.ds(0, LOCAL)], after, halo[2], halo[3])
    wait_bytes(tap_bf.at[pl.ds(0, 3), pl.ds(0, 2)], par_sems[1])
    for step in (1, 2, 3):
        other = (x + step) % 4
        ref = tap_bf.at[other, own_taps]
        send(ref, ref, sibling, par_sems[4], par_sems[5])
    sent.append((tap_bf.at[pl.ds(0, 3), pl.ds(0, 2)], par_sems[4]))

    ph1[0]()
    own(0, 0)
    own(0, 1)
    line_relay(2)
    line_relay(3)
    share_own(0)
    ph1[1]()
    own(1, 0)
    relay(0)
    own(1, 1)
    share_first(0)
    share_own(1)
    ph1[2]()
    own(2, 0)
    relay(1)
    own(2, 1)
    share_second(0)
    share_relay(0)
    share_first(1)
    share_own(2)
    ph1[3]()
    own(3, 0)

    wait_bytes(vec_all.at[pl.ds(0, 3)], par_sems[3])
    wait_bytes(tap_bf.at[pl.ds(0, 3), pl.ds(0, 2)], par_sems[5])
    tap_all[...] = tap_bf[...].astype(F32)
    gain_load.wait()
    for a_sem in halo:
        wait_bytes(x_buf.at[own_rows], a_sem)

    arrived(0)

    def middle0():
        relay(2)
        own(3, 1)

    compute(0, lambda: None)
    middle0()
    share_first(2)
    share_second(1)
    share_relay(1)
    share_own(3)
    arrived(1)
    compute(1, lambda: None)
    relay(3)
    share_first(3)
    share_second(2)
    share_relay(2)
    arrived(2)
    compute(2, lambda: share_second(3))
    share_relay(3)
    arrived(3)

    act = activated(3, lambda: None)
    end_send, end_recv = new_sem(), new_sem()
    for i, step in enumerate((2, 1, 3, 0)):
        other = (x + step) % 4
        cols = pl.ds(pl.multiple_of(other * 256, 256), 256)
        result = (x_buf[own_rows, cols].astype(F32) + branch(3, act, other)).astype(BF16)
        if step:
            y_buf[i] = result
            send(y_buf.at[i], out.at[x], (sp, other), end_send, end_recv)
        else:
            out[x] = result
    sent.append((y_buf.at[pl.ds(0, 3)], end_send))
    wait_bytes(y_buf.at[pl.ds(0, 3)], end_recv)
    for ref, a_sem in sent:
        wait_bytes(ref, a_sem)


def shards(tokens, norm_gain, val_w, gate_w, taps, bias, ln_gain, ln_shift, out_w):
    hbm = pl.BlockSpec(memory_space=pl.ANY)
    vmem = pl.BlockSpec(memory_space=pltpu.VMEM)
    return pl.pallas_call(
        kernel,
        out_shape=pltpu.VMEM(tokens.shape, BF16),
        in_specs=[hbm] * 9,
        out_specs=vmem,
        scratch_shapes=[
            pltpu.VMEM((LAYERS, 3, 2, 4, 4, 4, 32, 128), BF16),
            pltpu.VMEM((ROWS, 1024), BF16),
            pltpu.VMEM((ROWS, 512), F32),
            pltpu.VMEM((ROWS, 512), F32),
            pltpu.VMEM((ROWS, 1024), BF16),
            pltpu.VMEM((LAYERS, 1024), F32),
            pltpu.VMEM((TAPS, LAYERS, 128), F32),
            pltpu.VMEM((4, LAYERS, 32, 128), BF16),
            pltpu.VMEM((4, LAYERS, 32, 128), F32),
            pltpu.VMEM((4, 3, LAYERS, 128), F32),
            pltpu.VMEM((3, LOCAL, 256), BF16),
            pltpu.SemaphoreType.DMA((SEMS,)),
        ],
        compiler_params=pltpu.CompilerParams(collective_id=0, has_side_effects=True),
    )(
        tokens, norm_gain, val_w, gate_w, jnp.swapaxes(out_w, 1, 2),
        jnp.swapaxes(taps, 0, 1), bias, ln_gain, ln_shift,
    )


def solution(mesh):
    return jax.shard_map(
        shards,
        mesh=mesh,
        in_specs=(
            P(None, "sp", "tp"),
            P(),
            P(None, "sp", "tp"),
            P(None, "sp", "tp"),
            P(None, None, "tp"),
            P(None, "tp"),
            P(None, "tp"),
            P(None, "tp"),
            P(None, "tp", "sp"),
        ),
        out_specs=P(None, "sp", "tp"),
        check_vma=False,
    )
```

```python
import jax
import jax.numpy as jnp
from jax import lax
from jax.experimental import pallas as pl
from jax.experimental.pallas import tpu as pltpu
from jax.sharding import PartitionSpec as P

MESH = pl.DeviceIdType.MESH
LAYERS = 4
TAPS = 31
EPS = 1e-6
LOCAL = 64
ROWS = 192
STEP = 16
CYCLE = ("xyz", "yzx", "zxy")
ORDERS = (CYCLE, CYCLE, CYCLE, CYCLE)
SEMS = 280
F32 = jnp.float32
BF16 = jnp.bfloat16


def kernel(
    tokens, norm_gain, val_w, gate_w, out_w, taps, bias, ln_gain, ln_shift, out,
    w, x_buf, g_buf, c_buf, nb, gains, tap_in, tap_bf, tap_all, vec_all, y_buf, sem,
):
    sp = lax.axis_index("sp")
    x = lax.axis_index("tp")
    z = sp // 8
    y = (sp // 2) % 4
    c = sp % 2
    at = {"x": x, "y": y, "z": z}
    sibling = (sp + 1 - 2 * c, x)
    used = []

    def new_sem():
        used.append(0)
        return sem.at[len(used) - 1]

    def near(axis, step):
        if axis == "x":
            return (sp, (x + step) % 4)
        if axis == "y":
            return (z * 8 + ((y + step) % 4) * 2 + c, x)
        return (((z + step) % 4) * 8 + y * 2 + c, x)

    before = ((sp + 31) % 32, x)
    after = ((sp + 1) % 32, x)
    outer = ((sp + 31 + 2 * c) % 32, x)

    def send(ref, dst, peer, s_sem, r_sem):
        pltpu.make_async_remote_copy(
            src_ref=ref, dst_ref=dst, send_sem=s_sem, recv_sem=r_sem,
            device_id=peer, device_id_type=MESH,
        ).start()

    def wait_bytes(ref, a_sem):
        pltpu.make_async_copy(ref, ref, a_sem).wait()

    sent = []

    own_cols = pl.ds(pl.multiple_of(x * 256, 256), 256)
    own_rows = pl.ds(LOCAL, LOCAL)

    def load(src, dst):
        copy = pltpu.make_async_copy(src, dst, new_sem())
        copy.start()
        return copy

    loads = []
    for layer in range(LAYERS):
        for k, array in enumerate((val_w, gate_w, out_w)):
            d1, d2, d3 = ORDERS[layer][k]
            loads.append(load(array.at[layer], w.at[layer, k, c, at[d3], at[d2], at[d1]]))
    tap_load = load(taps, tap_in)
    small_loads = [
        load(array, vec_all.at[x, j]) for j, array in enumerate((bias, ln_gain, ln_shift))
    ]
    token_load = load(tokens.at[x], x_buf.at[own_rows, own_cols])
    gain_load = load(norm_gain, gains)

    barrier = pltpu.get_barrier_semaphore()
    peers = [near(a, s) for a in "xyz" for s in (1, 3, 2)] + [sibling, outer]
    for peer in peers:
        pl.semaphore_signal(barrier, inc=1, device_id=peer, device_id_type=MESH)

    tap_load.wait()
    for layer in range(LAYERS):
        tap_bf[x, layer] = jnp.concatenate(
            [tap_in[:, layer, :], jnp.zeros((1, 128), F32)], axis=0
        ).astype(BF16)
    for copy in loads:
        copy.wait()
    pl.semaphore_wait(barrier, len(peers))

    def block(k, phase, layer, index):
        d1, d2, d3 = ORDERS[layer][k]
        if phase == 0:
            return w.at[layer, k, c, at[d3], at[d2], index]
        if phase == 1:
            return w.at[layer, k, c, at[d3], index]
        return w.at[layer, k, c, index]

    def many(k, phase, layer, count):
        if phase == 0:
            return w.at[layer, k, 0, 0, 0, pl.ds(0, count)]
        if phase == 1:
            return w.at[layer, k, 0, 0, pl.ds(0, count)]
        return w.at[layer, k, 0, pl.ds(0, count)]

    def direct(phase, layer):
        waits = []
        for k in range(3):
            s_sem, r_sem = new_sem(), new_sem()
            axis = ORDERS[layer][k][phase]
            ref = block(k, phase, layer, at[axis])
            for step in (2, 1, 3):
                send(ref, ref, near(axis, step), s_sem, r_sem)
            sent.append((many(k, phase, layer, 3), s_sem))
            waits.append((many(k, phase, layer, 3), r_sem))

        def wait():
            for ref, r_sem in waits:
                wait_bytes(ref, r_sem)

        return wait

    line_sems = [[[new_sem(), new_sem()] for k in range(3)] for l in range(LAYERS)]
    line_rest = [[new_sem() for k in range(3)] for l in range(LAYERS)]
    line_send = [[new_sem() for k in range(3)] for l in range(LAYERS)]

    def line_half(k, layer, index, half):
        d1, d2, d3 = ORDERS[layer][k]
        return w.at[layer, k, c, at[d3], index, pl.ds(2 * half, 2)]

    def line_own(layer):
        for which in (0, 1):
            for k in range(3):
                axis = ORDERS[layer][k][1]
                for way in (0, 1):
                    half = which if way == 0 else 1 - which
                    ref = line_half(k, layer, at[axis], half)
                    r_sem = line_sems[layer][k][way] if which == 0 else line_rest[layer][k]
                    send(ref, ref, near(axis, 1 if way == 0 else 3), line_send[layer][k], r_sem)
        for k in range(3):
            sent.append((many(k, 1, layer, 3), line_send[layer][k]))

    def line_relay(layer):
        for k in range(3):
            axis = ORDERS[layer][k][1]
            for way in (0, 1):
                step = 1 if way == 0 else 3
                ref = line_half(k, layer, (at[axis] + 4 - step) % 4, way)
                wait_bytes(ref, line_sems[layer][k][way])
                send(ref, ref, near(axis, step), line_send[layer][k], line_rest[layer][k])

    def line_wait(layer):
        for k in range(3):
            wait_bytes(many(k, 1, layer, 2), line_rest[layer][k])

    first_sems = [[[new_sem(), new_sem()] for k in range(3)] for l in range(LAYERS)]
    second_sems = [[new_sem() for k in range(3)] for l in range(LAYERS)]
    relay_sems = [[new_sem() for k in range(3)] for l in range(LAYERS)]
    ring_send = [[new_sem() for k in range(3)] for l in range(LAYERS)]
    sib_send = [[new_sem() for k in range(3)] for l in range(LAYERS)]
    sib_recv = [[new_sem() for k in range(3)] for l in range(LAYERS)]
    for l in range(LAYERS):
        for k in range(3):
            sent.append((many(k, 2, l, 3), ring_send[l][k]))
            sent.append((many(k, 2, l, 4), sib_send[l][k]))

    def half_block(k, layer, index, half):
        return w.at[layer, k, c, index, pl.ds(2 * half, 2)]

    def to_sibling(k, layer, ref):
        send(ref, ref, sibling, sib_send[layer][k], sib_recv[layer][k])

    def own(layer, which):
        for k in range(3):
            axis = ORDERS[layer][k][2]
            for way in (0, 1):
                half = which if way == 0 else 1 - which
                ref = half_block(k, layer, at[axis], half)
                r_sem = first_sems[layer][k][way] if which == 0 else second_sems[layer][k]
                send(ref, ref, near(axis, 1 if way == 0 else 3), ring_send[layer][k], r_sem)

    def relay(layer):
        for k in range(3):
            axis = ORDERS[layer][k][2]
            for way in (0, 1):
                step = 1 if way == 0 else 3
                ref = half_block(k, layer, (at[axis] + 4 - step) % 4, way)
                wait_bytes(ref, first_sems[layer][k][way])
                send(ref, ref, near(axis, step), ring_send[layer][k], relay_sems[layer][k])

    def share_own(layer):
        for k in range(3):
            to_sibling(k, layer, block(k, 2, layer, at[ORDERS[layer][k][2]]))

    def share_first(layer):
        for k in range(3):
            axis = ORDERS[layer][k][2]
            for way in (0, 1):
                to_sibling(k, layer, half_block(k, layer, (at[axis] + (3, 1)[way]) % 4, way))

    def share_second(layer):
        for k in range(3):
            axis = ORDERS[layer][k][2]
            wait_bytes(many(k, 2, layer, 1), second_sems[layer][k])
            for way in (0, 1):
                to_sibling(k, layer, half_block(k, layer, (at[axis] + (3, 1)[way]) % 4, 1 - way))

    def share_relay(layer):
        for k in range(3):
            axis = ORDERS[layer][k][2]
            wait_bytes(many(k, 2, layer, 1), relay_sems[layer][k])
            to_sibling(k, layer, block(k, 2, layer, (at[axis] + 2) % 4))

    def arrived(layer):
        for k in range(3):
            wait_bytes(many(k, 2, layer, 4), sib_recv[layer][k])

    def weight(layer, k, bz, cols):
        def piece(by, bc, bx):
            index = {"x": bx, "y": by, "z": bz}
            d1, d2, d3 = ORDERS[layer][k]
            return w[layer, k, bc, index[d3], index[d2], index[d1]]

        return jnp.concatenate(
            [
                jnp.concatenate([piece(by, bc, bx) for by in range(4) for bc in range(2)], axis=0)
                for bx in cols
            ],
            axis=1,
        )

    def branch(layer, act, bz):
        return lax.dot_general(
            act, weight(layer, 2, bz, range(4)), (((1,), (1,)), ((), ())),
            preferred_element_type=F32,
        )

    def normed(layer):
        r0 = STEP * layer
        n = ROWS - 2 * r0
        xs = x_buf[pl.ds(r0, n), :].astype(F32)
        scale = lax.rsqrt(jnp.mean(xs * xs, axis=-1, keepdims=True) + EPS)
        nb[pl.ds(0, n), :] = (xs * scale * gains[pl.ds(layer, 1), :]).astype(BF16)

    def activated(layer, middle):
        r0 = STEP * layer
        n = ROWS - 2 * r0
        m = n - 2 * STEP
        token = sp * LOCAL - LOCAL + r0 + lax.broadcasted_iota(jnp.int32, (n, 256), 0)
        inside = jnp.logical_and(token >= 0, token < 32 * LOCAL)
        for half in range(2):
            cols = (2 * half, 2 * half + 1)
            val = jnp.zeros((n, 256), F32)
            gate = jnp.zeros((n, 256), F32)
            for bz in range(4):
                left = nb[pl.ds(0, n), pl.ds(bz * 256, 256)]
                val = val + jnp.dot(left, weight(layer, 0, bz, cols), preferred_element_type=F32)
                gate = gate + jnp.dot(left, weight(layer, 1, bz, cols), preferred_element_type=F32)
            gated = (val * jax.nn.sigmoid(gate)).astype(BF16).astype(F32)
            g_buf[pl.ds(0, n), pl.ds(half * 256, 256)] = jnp.where(inside, gated, 0.0)
        for bx in range(4):
            lanes = pl.ds(bx * 128, 128)
            g = g_buf[pl.ds(0, n), lanes]
            total = jnp.zeros((m, 128), F32) + vec_all[bx, 0, pl.ds(layer, 1), :]
            for shift in range(8):
                moved = g if shift == 0 else pltpu.roll(g, n - shift, 0)
                for k in range(TAPS):
                    if (k + 1) % 8 == shift:
                        base = (k + 1) // 8 * 8
                        total = total + moved[base : base + m] * tap_all[bx, layer, pl.ds(k, 1), :]
            c_buf[pl.ds(0, m), lanes] = total
        middle()
        conv = c_buf[pl.ds(0, m), :]
        mean = jnp.mean(conv, axis=-1, keepdims=True)
        centred = conv - mean
        spread = jnp.mean(centred * centred, axis=-1, keepdims=True)
        gain = jnp.concatenate([vec_all[bx, 1, pl.ds(layer, 1), :] for bx in range(4)], axis=1)
        shift = jnp.concatenate([vec_all[bx, 2, pl.ds(layer, 1), :] for bx in range(4)], axis=1)
        normalized = centred * lax.rsqrt(spread + EPS) * gain + shift
        return jax.nn.silu(normalized).astype(BF16)

    def compute(layer, middle):
        act = activated(layer, middle)
        rows = pl.ds(STEP * (layer + 1), ROWS - 2 * STEP * (layer + 1))
        for bz in range(4):
            lanes = pl.ds(bz * 256, 256)
            x_buf[rows, lanes] = (x_buf[rows, lanes].astype(F32) + branch(layer, act, bz)).astype(BF16)

    ph0 = [direct(0, layer) for layer in range(LAYERS)]

    tok_send, tok_recv = new_sem(), new_sem()
    for step in (2, 1, 3):
        other = (x + step) % 4
        send(tokens.at[other], x_buf.at[own_rows, own_cols], (sp, other), tok_send, tok_recv)
    sent.append((x_buf.at[own_rows, pl.ds(0, 768)], tok_send))
    own_taps = pl.ds(2 * c, 2)
    par_sems = [new_sem() for _ in range(6)]
    for copy in small_loads:
        copy.wait()
    for step in (2, 1, 3):
        other = (x + step) % 4
        send(tap_bf.at[x, own_taps], tap_bf.at[x, own_taps], (sp, other), par_sems[0], par_sems[1])
        send(vec_all.at[x], vec_all.at[x], (sp, other), par_sems[2], par_sems[3])
    sent.append((tap_bf.at[pl.ds(0, 3), pl.ds(0, 2)], par_sems[0]))
    sent.append((vec_all.at[pl.ds(0, 3)], par_sems[2]))

    ph1 = []
    for layer in range(LAYERS):
        ph0[layer]()
        if layer in (2, 3):
            line_own(layer)
            ph1.append(lambda layer=layer: line_wait(layer))
        else:
            ph1.append(direct(1, layer))

    token_load.wait()
    wait_bytes(x_buf.at[own_rows, pl.ds(0, 768)], tok_recv)
    halo = [new_sem() for _ in range(4)]
    send(x_buf.at[own_rows], x_buf.at[pl.ds(2 * LOCAL, LOCAL)], before, halo[0], halo[1])
    send(x_buf.at[own_rows], x_buf.at[pl.ds(0, LOCAL)], after, halo[2], halo[3])
    wait_bytes(tap_bf.at[pl.ds(0, 3), pl.ds(0, 2)], par_sems[1])
    for step in (1, 2, 3):
        other = (x + step) % 4
        ref = tap_bf.at[other, own_taps]
        send(ref, ref, sibling, par_sems[4], par_sems[5])
    sent.append((tap_bf.at[pl.ds(0, 3), pl.ds(0, 2)], par_sems[4]))

    ph1[0]()
    own(0, 0)
    own(0, 1)
    line_relay(2)
    line_relay(3)
    share_own(0)
    ph1[1]()
    own(1, 0)
    relay(0)
    own(1, 1)
    share_first(0)
    share_own(1)
    ph1[2]()
    own(2, 0)
    relay(1)
    own(2, 1)
    share_second(0)
    share_relay(0)
    share_first(1)
    share_own(2)
    ph1[3]()
    own(3, 0)

    wait_bytes(vec_all.at[pl.ds(0, 3)], par_sems[3])
    wait_bytes(tap_bf.at[pl.ds(0, 3), pl.ds(0, 2)], par_sems[5])
    tap_all[...] = tap_bf[...].astype(F32)
    gain_load.wait()
    for a_sem in halo:
        wait_bytes(x_buf.at[own_rows], a_sem)

    normed(0)
    arrived(0)

    def middle0():
        relay(2)
        own(3, 1)

    compute(0, lambda: None)
    middle0()
    share_first(2)
    share_second(1)
    share_relay(1)
    share_own(3)
    normed(1)
    arrived(1)
    relay(3)
    share_second(2)
    share_first(3)
    compute(1, lambda: None)
    share_relay(2)
    normed(2)
    arrived(2)
    compute(2, lambda: share_second(3))
    share_relay(3)
    normed(3)
    arrived(3)

    act = activated(3, lambda: None)
    end_send, end_recv = new_sem(), new_sem()
    for i, step in enumerate((2, 1, 3, 0)):
        other = (x + step) % 4
        cols = pl.ds(pl.multiple_of(other * 256, 256), 256)
        result = (x_buf[own_rows, cols].astype(F32) + branch(3, act, other)).astype(BF16)
        if step:
            y_buf[i] = result
            send(y_buf.at[i], out.at[x], (sp, other), end_send, end_recv)
        else:
            out[x] = result
    sent.append((y_buf.at[pl.ds(0, 3)], end_send))
    wait_bytes(y_buf.at[pl.ds(0, 3)], end_recv)
    for ref, a_sem in sent:
        wait_bytes(ref, a_sem)


def shards(tokens, norm_gain, val_w, gate_w, taps, bias, ln_gain, ln_shift, out_w):
    hbm = pl.BlockSpec(memory_space=pl.ANY)
    vmem = pl.BlockSpec(memory_space=pltpu.VMEM)
    return pl.pallas_call(
        kernel,
        out_shape=pltpu.VMEM(tokens.shape, BF16),
        in_specs=[hbm] * 9,
        out_specs=vmem,
        scratch_shapes=[
            pltpu.VMEM((LAYERS, 3, 2, 4, 4, 4, 32, 128), BF16),
            pltpu.VMEM((ROWS, 1024), BF16),
            pltpu.VMEM((ROWS, 512), F32),
            pltpu.VMEM((ROWS, 512), F32),
            pltpu.VMEM((ROWS, 1024), BF16),
            pltpu.VMEM((LAYERS, 1024), F32),
            pltpu.VMEM((TAPS, LAYERS, 128), F32),
            pltpu.VMEM((4, LAYERS, 32, 128), BF16),
            pltpu.VMEM((4, LAYERS, 32, 128), F32),
            pltpu.VMEM((4, 3, LAYERS, 128), F32),
            pltpu.VMEM((3, LOCAL, 256), BF16),
            pltpu.SemaphoreType.DMA((SEMS,)),
        ],
        compiler_params=pltpu.CompilerParams(collective_id=0, has_side_effects=True),
    )(
        tokens, norm_gain, val_w, gate_w, jnp.swapaxes(out_w, 1, 2),
        jnp.swapaxes(taps, 0, 1), bias, ln_gain, ln_shift,
    )


def solution(mesh):
    return jax.shard_map(
        shards,
        mesh=mesh,
        in_specs=(
            P(None, "sp", "tp"),
            P(),
            P(None, "sp", "tp"),
            P(None, "sp", "tp"),
            P(None, None, "tp"),
            P(None, "tp"),
            P(None, "tp"),
            P(None, "tp"),
            P(None, "tp", "sp"),
        ),
        out_specs=P(None, "sp", "tp"),
        check_vma=False,
    )
```

```python
import jax
import jax.numpy as jnp
from jax import lax
from jax.experimental import pallas as pl
from jax.experimental.pallas import tpu as pltpu
from jax.sharding import PartitionSpec as P

MESH = pl.DeviceIdType.MESH
LAYERS = 4
TAPS = 31
EPS = 1e-6
LOCAL = 64
ROWS = 192
STEP = 16
CYCLE = ("xyz", "yzx", "zxy")
ORDERS = (CYCLE, CYCLE, CYCLE, CYCLE)
SEMS = 280
F32 = jnp.float32
BF16 = jnp.bfloat16


def kernel(
    tokens, norm_gain, val_w, gate_w, out_w, taps, bias, ln_gain, ln_shift, out,
    w, x_buf, g_buf, c_buf, nb, gains, tap_in, tap_bf, tap_all, vec_all, y_buf, sem,
):
    sp = lax.axis_index("sp")
    x = lax.axis_index("tp")
    z = sp // 8
    y = (sp // 2) % 4
    c = sp % 2
    at = {"x": x, "y": y, "z": z}
    sibling = (sp + 1 - 2 * c, x)
    used = []

    def new_sem():
        used.append(0)
        return sem.at[len(used) - 1]

    def near(axis, step):
        if axis == "x":
            return (sp, (x + step) % 4)
        if axis == "y":
            return (z * 8 + ((y + step) % 4) * 2 + c, x)
        return (((z + step) % 4) * 8 + y * 2 + c, x)

    before = ((sp + 31) % 32, x)
    after = ((sp + 1) % 32, x)
    outer = ((sp + 31 + 2 * c) % 32, x)

    def send(ref, dst, peer, s_sem, r_sem):
        pltpu.make_async_remote_copy(
            src_ref=ref, dst_ref=dst, send_sem=s_sem, recv_sem=r_sem,
            device_id=peer, device_id_type=MESH,
        ).start()

    def wait_bytes(ref, a_sem):
        pltpu.make_async_copy(ref, ref, a_sem).wait()

    sent = []

    own_cols = pl.ds(pl.multiple_of(x * 256, 256), 256)
    own_rows = pl.ds(LOCAL, LOCAL)

    def load(src, dst):
        copy = pltpu.make_async_copy(src, dst, new_sem())
        copy.start()
        return copy

    loads = []
    for layer in range(LAYERS):
        for k, array in enumerate((val_w, gate_w, out_w)):
            d1, d2, d3 = ORDERS[layer][k]
            loads.append(load(array.at[layer], w.at[layer, k, c, at[d3], at[d2], at[d1]]))
    tap_load = load(taps, tap_in)
    small_loads = [
        load(array, vec_all.at[x, j]) for j, array in enumerate((bias, ln_gain, ln_shift))
    ]
    token_load = load(tokens.at[x], x_buf.at[own_rows, own_cols])
    gain_load = load(norm_gain, gains)

    barrier = pltpu.get_barrier_semaphore()
    peers = [near(a, s) for a in "xyz" for s in (1, 3, 2)] + [sibling, outer]
    for peer in peers:
        pl.semaphore_signal(barrier, inc=1, device_id=peer, device_id_type=MESH)

    for copy in loads[:3]:
        copy.wait()
    pl.semaphore_wait(barrier, len(peers))

    def block(k, phase, layer, index):
        d1, d2, d3 = ORDERS[layer][k]
        if phase == 0:
            return w.at[layer, k, c, at[d3], at[d2], index]
        if phase == 1:
            return w.at[layer, k, c, at[d3], index]
        return w.at[layer, k, c, index]

    def many(k, phase, layer, count):
        if phase == 0:
            return w.at[layer, k, 0, 0, 0, pl.ds(0, count)]
        if phase == 1:
            return w.at[layer, k, 0, 0, pl.ds(0, count)]
        return w.at[layer, k, 0, pl.ds(0, count)]

    def direct(phase, layer):
        waits = []
        for k in range(3):
            s_sem, r_sem = new_sem(), new_sem()
            axis = ORDERS[layer][k][phase]
            ref = block(k, phase, layer, at[axis])
            for step in (2, 1, 3):
                send(ref, ref, near(axis, step), s_sem, r_sem)
            sent.append((many(k, phase, layer, 3), s_sem))
            waits.append((many(k, phase, layer, 3), r_sem))

        def wait():
            for ref, r_sem in waits:
                wait_bytes(ref, r_sem)

        return wait

    line_sems = [[[new_sem(), new_sem()] for k in range(3)] for l in range(LAYERS)]
    line_rest = [[new_sem() for k in range(3)] for l in range(LAYERS)]
    line_send = [[new_sem() for k in range(3)] for l in range(LAYERS)]

    def line_half(k, layer, index, half):
        d1, d2, d3 = ORDERS[layer][k]
        return w.at[layer, k, c, at[d3], index, pl.ds(2 * half, 2)]

    def line_own(layer):
        for which in (0, 1):
            for k in range(3):
                axis = ORDERS[layer][k][1]
                for way in (0, 1):
                    half = which if way == 0 else 1 - which
                    ref = line_half(k, layer, at[axis], half)
                    r_sem = line_sems[layer][k][way] if which == 0 else line_rest[layer][k]
                    send(ref, ref, near(axis, 1 if way == 0 else 3), line_send[layer][k], r_sem)
        for k in range(3):
            sent.append((many(k, 1, layer, 3), line_send[layer][k]))

    def line_relay(layer):
        for k in range(3):
            axis = ORDERS[layer][k][1]
            for way in (0, 1):
                step = 1 if way == 0 else 3
                ref = line_half(k, layer, (at[axis] + 4 - step) % 4, way)
                wait_bytes(ref, line_sems[layer][k][way])
                send(ref, ref, near(axis, step), line_send[layer][k], line_rest[layer][k])

    def line_wait(layer):
        for k in range(3):
            wait_bytes(many(k, 1, layer, 2), line_rest[layer][k])

    first_sems = [[[new_sem(), new_sem()] for k in range(3)] for l in range(LAYERS)]
    second_sems = [[new_sem() for k in range(3)] for l in range(LAYERS)]
    relay_sems = [[new_sem() for k in range(3)] for l in range(LAYERS)]
    ring_send = [[new_sem() for k in range(3)] for l in range(LAYERS)]
    sib_send = [[new_sem() for k in range(3)] for l in range(LAYERS)]
    sib_recv = [[new_sem() for k in range(3)] for l in range(LAYERS)]
    for l in range(LAYERS):
        for k in range(3):
            sent.append((many(k, 2, l, 3), ring_send[l][k]))
            sent.append((many(k, 2, l, 4), sib_send[l][k]))
    late_sems = [new_sem() for k in range(3)]

    def half_block(k, layer, index, half):
        return w.at[layer, k, c, index, pl.ds(2 * half, 2)]

    def to_sibling(k, layer, ref, late=False):
        r_sem = late_sems[k] if late and layer == 3 else sib_recv[layer][k]
        send(ref, ref, sibling, sib_send[layer][k], r_sem)

    def own(layer, which):
        for k in range(3):
            axis = ORDERS[layer][k][2]
            for way in (0, 1):
                half = which if way == 0 else 1 - which
                ref = half_block(k, layer, at[axis], half)
                r_sem = first_sems[layer][k][way] if which == 0 else second_sems[layer][k]
                send(ref, ref, near(axis, 1 if way == 0 else 3), ring_send[layer][k], r_sem)

    def relay(layer):
        for k in range(3):
            axis = ORDERS[layer][k][2]
            for way in (0, 1):
                step = 1 if way == 0 else 3
                ref = half_block(k, layer, (at[axis] + 4 - step) % 4, way)
                wait_bytes(ref, first_sems[layer][k][way])
                send(ref, ref, near(axis, step), ring_send[layer][k], relay_sems[layer][k])

    def share_own(layer):
        for k in range(3):
            to_sibling(k, layer, block(k, 2, layer, at[ORDERS[layer][k][2]]))

    def share_first(layer):
        for k in range(3):
            axis = ORDERS[layer][k][2]
            for way in (0, 1):
                to_sibling(k, layer, half_block(k, layer, (at[axis] + (3, 1)[way]) % 4, way))

    def share_second(layer):
        for k in range(3):
            axis = ORDERS[layer][k][2]
            wait_bytes(many(k, 2, layer, 1), second_sems[layer][k])
            for way in (0, 1):
                to_sibling(k, layer, half_block(k, layer, (at[axis] + (3, 1)[way]) % 4, 1 - way))

    def share_relay(layer):
        for k in range(3):
            axis = ORDERS[layer][k][2]
            wait_bytes(many(k, 2, layer, 1), relay_sems[layer][k])
            to_sibling(k, layer, block(k, 2, layer, (at[axis] + 2) % 4), late=True)

    def arrived(layer):
        for k in range(3):
            wait_bytes(many(k, 2, layer, 3 if layer == 3 else 4), sib_recv[layer][k])

    def weight(layer, k, bz, cols):
        def piece(by, bc, bx):
            index = {"x": bx, "y": by, "z": bz}
            d1, d2, d3 = ORDERS[layer][k]
            return w[layer, k, bc, index[d3], index[d2], index[d1]]

        return jnp.concatenate(
            [
                jnp.concatenate([piece(by, bc, bx) for by in range(4) for bc in range(2)], axis=0)
                for bx in cols
            ],
            axis=1,
        )

    def left(n, bz):
        return nb[pl.ds(0, n), pl.ds(pl.multiple_of(bz * 256, 256), 256)]

    last = ROWS - 2 * STEP * 3
    every = pl.ds(0, last)

    def gate_block(bx):
        total = jnp.zeros((last, 128), F32)
        for bz in range(4):
            total = total + jnp.dot(
                left(last, bz), weight(3, 1, bz, (bx,)), preferred_element_type=F32
            )
        g_buf[every, pl.ds(pl.multiple_of(bx * 128, 128), 128)] = total

    def last_early():
        total = jnp.zeros((last, 512), F32)
        for step in (0, 1, 3):
            bz = (z + step) % 4
            total = total + jnp.dot(
                left(last, bz), weight(3, 0, bz, range(4)), preferred_element_type=F32
            )
        c_buf[every, :] = total
        for step in (0, 1, 3):
            gate_block((x + step) % 4)

    def last_late():
        bz = (z + 2) % 4
        gate_block((x + 2) % 4)
        for half in range(2):
            lanes = pl.ds(half * 256, 256)
            c_buf[every, lanes] = c_buf[every, lanes] + jnp.dot(
                left(last, bz), weight(3, 0, bz, (2 * half, 2 * half + 1)), preferred_element_type=F32
            )

    def branch(layer, act, bz):
        return lax.dot_general(
            act, weight(layer, 2, bz, range(4)), (((1,), (1,)), ((), ())),
            preferred_element_type=F32,
        )

    def normed(layer):
        r0 = STEP * layer
        n = ROWS - 2 * r0
        xs = x_buf[pl.ds(r0, n), :].astype(F32)
        scale = lax.rsqrt(jnp.mean(xs * xs, axis=-1, keepdims=True) + EPS)
        nb[pl.ds(0, n), :] = (xs * scale * gains[pl.ds(layer, 1), :]).astype(BF16)

    def activated(layer, middle):
        r0 = STEP * layer
        n = ROWS - 2 * r0
        m = n - 2 * STEP
        token = sp * LOCAL - LOCAL + r0 + lax.broadcasted_iota(jnp.int32, (n, 256), 0)
        inside = jnp.logical_and(token >= 0, token < 32 * LOCAL)
        for half in range(2):
            cols = (2 * half, 2 * half + 1)
            if layer == 3:
                val = c_buf[pl.ds(0, n), pl.ds(half * 256, 256)]
                gate = g_buf[pl.ds(0, n), pl.ds(half * 256, 256)]
            else:
                val = jnp.zeros((n, 256), F32)
                gate = jnp.zeros((n, 256), F32)
                for bz in range(4):
                    part = left(n, bz)
                    val = val + jnp.dot(part, weight(layer, 0, bz, cols), preferred_element_type=F32)
                    gate = gate + jnp.dot(part, weight(layer, 1, bz, cols), preferred_element_type=F32)
            gated = (val * jax.nn.sigmoid(gate)).astype(BF16).astype(F32)
            g_buf[pl.ds(0, n), pl.ds(half * 256, 256)] = jnp.where(inside, gated, 0.0)
        for bx in range(4):
            lanes = pl.ds(bx * 128, 128)
            g = g_buf[pl.ds(0, n), lanes]
            total = jnp.zeros((m, 128), F32) + vec_all[bx, 0, pl.ds(layer, 1), :]
            for shift in range(8):
                moved = g if shift == 0 else pltpu.roll(g, n - shift, 0)
                for k in range(TAPS):
                    if (k + 1) % 8 == shift:
                        base = (k + 1) // 8 * 8
                        total = total + moved[base : base + m] * tap_all[bx, layer, pl.ds(k, 1), :]
            c_buf[pl.ds(0, m), lanes] = total
        middle()
        conv = c_buf[pl.ds(0, m), :]
        mean = jnp.mean(conv, axis=-1, keepdims=True)
        centred = conv - mean
        spread = jnp.mean(centred * centred, axis=-1, keepdims=True)
        gain = jnp.concatenate([vec_all[bx, 1, pl.ds(layer, 1), :] for bx in range(4)], axis=1)
        shift = jnp.concatenate([vec_all[bx, 2, pl.ds(layer, 1), :] for bx in range(4)], axis=1)
        normalized = centred * lax.rsqrt(spread + EPS) * gain + shift
        return jax.nn.silu(normalized).astype(BF16)

    def compute(layer, middle):
        act = activated(layer, middle)
        rows = pl.ds(STEP * (layer + 1), ROWS - 2 * STEP * (layer + 1))
        for bz in range(4):
            lanes = pl.ds(bz * 256, 256)
            x_buf[rows, lanes] = (x_buf[rows, lanes].astype(F32) + branch(layer, act, bz)).astype(BF16)

    ph0 = [direct(0, 0)]
    for copy in loads[3:]:
        copy.wait()
    ph0 += [direct(0, layer) for layer in range(1, LAYERS)]
    tap_load.wait()
    for layer in range(LAYERS):
        tap_bf[x, layer] = jnp.concatenate(
            [tap_in[:, layer, :], jnp.zeros((1, 128), F32)], axis=0
        ).astype(BF16)

    tok_send, tok_recv = new_sem(), new_sem()
    for step in (2, 1, 3):
        other = (x + step) % 4
        send(tokens.at[other], x_buf.at[own_rows, own_cols], (sp, other), tok_send, tok_recv)
    sent.append((x_buf.at[own_rows, pl.ds(0, 768)], tok_send))
    own_taps = pl.ds(2 * c, 2)
    par_sems = [new_sem() for _ in range(6)]
    for copy in small_loads:
        copy.wait()
    for step in (2, 1, 3):
        other = (x + step) % 4
        send(tap_bf.at[x, own_taps], tap_bf.at[x, own_taps], (sp, other), par_sems[0], par_sems[1])
        send(vec_all.at[x], vec_all.at[x], (sp, other), par_sems[2], par_sems[3])
    sent.append((tap_bf.at[pl.ds(0, 3), pl.ds(0, 2)], par_sems[0]))
    sent.append((vec_all.at[pl.ds(0, 3)], par_sems[2]))

    ph1 = []
    for layer in range(LAYERS):
        ph0[layer]()
        if layer in (2, 3):
            line_own(layer)
            ph1.append(lambda layer=layer: line_wait(layer))
        else:
            ph1.append(direct(1, layer))

    token_load.wait()
    wait_bytes(x_buf.at[own_rows, pl.ds(0, 768)], tok_recv)
    halo = [new_sem() for _ in range(4)]
    send(x_buf.at[own_rows], x_buf.at[pl.ds(2 * LOCAL, LOCAL)], before, halo[0], halo[1])
    send(x_buf.at[own_rows], x_buf.at[pl.ds(0, LOCAL)], after, halo[2], halo[3])
    wait_bytes(tap_bf.at[pl.ds(0, 3), pl.ds(0, 2)], par_sems[1])
    for step in (1, 2, 3):
        other = (x + step) % 4
        ref = tap_bf.at[other, own_taps]
        send(ref, ref, sibling, par_sems[4], par_sems[5])
    sent.append((tap_bf.at[pl.ds(0, 3), pl.ds(0, 2)], par_sems[4]))

    ph1[0]()
    own(0, 0)
    own(0, 1)
    line_relay(2)
    line_relay(3)
    share_own(0)
    ph1[1]()
    own(1, 0)
    relay(0)
    own(1, 1)
    share_first(0)
    share_own(1)
    ph1[2]()
    own(2, 0)
    relay(1)
    own(2, 1)
    share_second(0)
    share_relay(0)
    share_first(1)
    share_own(2)
    ph1[3]()
    own(3, 0)

    wait_bytes(vec_all.at[pl.ds(0, 3)], par_sems[3])
    wait_bytes(tap_bf.at[pl.ds(0, 3), pl.ds(0, 2)], par_sems[5])
    tap_all[...] = tap_bf[...].astype(F32)
    gain_load.wait()
    for a_sem in halo:
        wait_bytes(x_buf.at[own_rows], a_sem)

    normed(0)
    arrived(0)

    def middle0():
        relay(2)
        own(3, 1)

    compute(0, lambda: None)
    middle0()
    share_first(2)
    share_second(1)
    share_relay(1)
    share_own(3)
    normed(1)
    arrived(1)
    relay(3)
    share_second(2)
    share_first(3)
    compute(1, lambda: None)
    share_relay(2)
    normed(2)
    arrived(2)
    share_second(3)
    compute(2, lambda: None)
    normed(3)
    share_relay(3)
    arrived(3)
    last_early()
    for k in (1, 0):
        wait_bytes(many(k, 2, 3, 1), late_sems[k])
    last_late()

    act = activated(3, lambda: None)
    wait_bytes(many(2, 2, 3, 1), late_sems[2])
    end_send, end_recv = new_sem(), new_sem()
    for i, step in enumerate((2, 1, 3, 0)):
        other = (x + step) % 4
        cols = pl.ds(pl.multiple_of(other * 256, 256), 256)
        result = (x_buf[own_rows, cols].astype(F32) + branch(3, act, other)).astype(BF16)
        if step:
            y_buf[i] = result
            send(y_buf.at[i], out.at[x], (sp, other), end_send, end_recv)
        else:
            out[x] = result
    for ref, a_sem in sent:
        wait_bytes(ref, a_sem)
    wait_bytes(y_buf.at[pl.ds(0, 3)], end_send)
    wait_bytes(y_buf.at[pl.ds(0, 3)], end_recv)


def shards(tokens, norm_gain, val_w, gate_w, taps, bias, ln_gain, ln_shift, out_w):
    hbm = pl.BlockSpec(memory_space=pl.ANY)
    vmem = pl.BlockSpec(memory_space=pltpu.VMEM)
    return pl.pallas_call(
        kernel,
        out_shape=pltpu.VMEM(tokens.shape, BF16),
        in_specs=[hbm] * 9,
        out_specs=vmem,
        scratch_shapes=[
            pltpu.VMEM((LAYERS, 3, 2, 4, 4, 4, 32, 128), BF16),
            pltpu.VMEM((ROWS, 1024), BF16),
            pltpu.VMEM((ROWS, 512), F32),
            pltpu.VMEM((ROWS, 512), F32),
            pltpu.VMEM((ROWS, 1024), BF16),
            pltpu.VMEM((LAYERS, 1024), F32),
            pltpu.VMEM((TAPS, LAYERS, 128), F32),
            pltpu.VMEM((4, LAYERS, 32, 128), BF16),
            pltpu.VMEM((4, LAYERS, 32, 128), F32),
            pltpu.VMEM((4, 3, LAYERS, 128), F32),
            pltpu.VMEM((3, LOCAL, 256), BF16),
            pltpu.SemaphoreType.DMA((SEMS,)),
        ],
        compiler_params=pltpu.CompilerParams(collective_id=0, has_side_effects=True),
    )(
        tokens, norm_gain, val_w, gate_w, jnp.swapaxes(out_w, 1, 2),
        jnp.swapaxes(taps, 0, 1), bias, ln_gain, ln_shift,
    )


def solution(mesh):
    return jax.shard_map(
        shards,
        mesh=mesh,
        in_specs=(
            P(None, "sp", "tp"),
            P(),
            P(None, "sp", "tp"),
            P(None, "sp", "tp"),
            P(None, None, "tp"),
            P(None, "tp"),
            P(None, "tp"),
            P(None, "tp"),
            P(None, "tp", "sp"),
        ),
        out_specs=P(None, "sp", "tp"),
        check_vma=False,
    )
```
